32 devices in a mesh: sp: 8 (over z, y), tp: 4 (over x, core).
Axes of the slice: x: 2, y: 2, z: 4, core: 2. Of those that a mesh axis runs over, the one named last changes fastest.
Arguments:
- layer_grad: bfloat16 [1536, 2048], P('sp'), may hold values from -6 to 6
- routes: int32 [1536, 2], P('sp'), may hold values from 0 to 7, as said below
- route_weight: float32 [1536, 2], P('sp'), may hold values from 0.1 to 0.9
- slot_tokens: bfloat16 [8, 576, 2048], P('sp'), may hold values from -6 to 6
- gate_proj: bfloat16 [8, 2048, 1024], P('sp', None, 'tp'), may hold values from -0.125 to 0.125
- up_proj: bfloat16 [8, 2048, 1024], P('sp', None, 'tp'), may hold values from -0.125 to 0.125
- down_proj: bfloat16 [8, 1024, 2048], P('sp', 'tp'), may hold values from -0.1875 to 0.1875
- out_proj: bfloat16 [2048, 1024], P(None, 'tp'), may hold values from -0.1875 to 0.1875
- queries: bfloat16 [1536, 512], P('sp', 'tp'), may hold values from -6 to 6
- keys: bfloat16 [1536, 512], P('sp', 'tp'), may hold values from -6 to 6
- values: bfloat16 [1536, 1024], P('sp', 'tp'), may hold values from -6 to 6
- fwd_decay: float32 [1536, 512], P('sp', 'tp'), may hold values from -2 to 0
- bwd_decay: float32 [1536, 512], P('sp', 'tp'), may hold values from -2 to 0
Outputs:
- gate_grad: bfloat16 [8, 2048, 1024], P('sp', None, 'tp')
- up_grad: bfloat16 [8, 2048, 1024], P('sp', None, 'tp')
- down_grad: bfloat16 [8, 1024, 2048], P('sp', 'tp')
- proj_grad: float32 [2048, 1024], P('sp', 'tp')
- query_grad: bfloat16 [1536, 512], P('sp', 'tp')
- key_grad: bfloat16 [1536, 512], P('sp', 'tp')
- value_grad: bfloat16 [1536, 1024], P('sp', 'tp')
The draws below stay inside these ranges and needn't reach their ends.
Inputs may be any that keep to these rules, and one draw needn't show every extreme that they name: `routes`: each row names two different experts of one group of 8 consecutive experts. In every aligned block of 192 rows one expert is named by 72 rows or more.
All inputs are finite; a program needn't handle non-finite values.
Results may differ from the reference program's by a relative error of at most 0.015.
Values may be sent and summed in bfloat16 or wider, within the bound.
A program may use at most 128 MiB of HBM per device.

```python
import functools
import jax
import jax.numpy as jnp
from jax import lax

D = 2048
ATTENTION_HEADS = 8
KEY_CHANNELS = 64
DV = 128
FF = 1024
EXP_GROUP = 8
BLOCK = 64
TOK_DEV = 192
EXPERTS = 8
CAP = 72
SLOTS = 576
SEQUENCE_TOKENS = 1536
N_SP = 8
N_TP = 4


def draw_routes(key, part):
    random_subkeys = jax.random.split(jax.random.fold_in(key, 11), 6)
    blocks = SEQUENCE_TOKENS // TOK_DEV
    group_count = EXPERTS // EXP_GROUP
    chosen_group = jax.random.randint(random_subkeys[0], (SEQUENCE_TOKENS,), 0, group_count)
    primary = jax.random.randint(random_subkeys[1], (SEQUENCE_TOKENS,), 0, EXP_GROUP)
    offsets = jax.random.randint(random_subkeys[2], (SEQUENCE_TOKENS,), 1, EXP_GROUP)
    hottest = jax.random.randint(random_subkeys[3], (), 0, EXPERTS)
    orders = jax.vmap(jax.random.permutation, in_axes=(0, None))(jax.random.split(random_subkeys[4], blocks), TOK_DEV)
    forced = (orders < CAP).reshape(SEQUENCE_TOKENS)
    chosen_group = jnp.where(forced, hottest // EXP_GROUP, chosen_group)
    primary = jnp.where(forced, hottest % EXP_GROUP, primary)
    secondary = (primary + offsets) % EXP_GROUP
    flipped = jax.random.randint(random_subkeys[5], (SEQUENCE_TOKENS,), 0, 2)
    first_id = chosen_group * EXP_GROUP + primary
    second_id = chosen_group * EXP_GROUP + secondary
    leading = jnp.where(flipped == 1, second_id, first_id)
    trailing = jnp.where(flipped == 1, first_id, second_id)
    return jnp.stack([leading, trailing], axis=1).astype(jnp.int32)


def decay_law(key, salt):
    random_subkeys = jax.random.split(jax.random.fold_in(key, salt), 12)
    blocks = SEQUENCE_TOKENS // TOK_DEV
    head_chance = 0.5
    block_chance = 0.5
    heads_index = jnp.arange(ATTENTION_HEADS)
    forced_head = jax.random.randint(random_subkeys[0], (), 0, ATTENTION_HEADS)
    steady_head = (forced_head + jax.random.randint(random_subkeys[1], (), 1, ATTENTION_HEADS)) % ATTENTION_HEADS
    mixed_head = jax.random.uniform(random_subkeys[2], (ATTENTION_HEADS,)) < head_chance
    mixed_head = jnp.logical_and(jnp.logical_or(mixed_head, heads_index == forced_head), heads_index != steady_head)
    fast_block = jax.random.uniform(random_subkeys[3], (blocks, ATTENTION_HEADS)) < block_chance
    turning = jax.random.randint(random_subkeys[4], (), 1, blocks)
    block_index = jnp.arange(blocks)[:, None]
    at_forced = (heads_index == forced_head)[None, :]
    fast_block = jnp.where(jnp.logical_and(block_index == turning, at_forced), True, fast_block)
    fast_block = jnp.where(jnp.logical_and(block_index == turning - 1, at_forced), False, fast_block)
    speedy = jnp.logical_and(fast_block, mixed_head[None, :])
    quick_rate = jax.random.uniform(random_subkeys[5], (ATTENTION_HEADS, KEY_CHANNELS), minval=0.02, maxval=0.035)
    slow_rate = jnp.exp(jax.random.uniform(random_subkeys[6], (ATTENTION_HEADS, KEY_CHANNELS), minval=-1.6, maxval=0.0)) / SEQUENCE_TOKENS
    rate_table = jnp.where(speedy[:, None, :, None], quick_rate[None, None], slow_rate[None, None])
    device_factor = jnp.exp(jax.random.uniform(random_subkeys[7], (blocks, 1, 1, 1), minval=-0.69, maxval=0.69))
    jitter = jax.random.uniform(random_subkeys[8], (blocks, TOK_DEV, ATTENTION_HEADS, KEY_CHANNELS), minval=0.4, maxval=1.6)
    steady_decay = -(rate_table * device_factor * jitter).reshape(SEQUENCE_TOKENS, ATTENTION_HEADS, KEY_CHANNELS)
    start_spike = jax.random.randint(random_subkeys[9], (ATTENTION_HEADS, 1), 0, blocks) * TOK_DEV
    free_spike = jax.random.randint(random_subkeys[10], (ATTENTION_HEADS, 1), 0, SEQUENCE_TOKENS)
    spike_position = jnp.concatenate([start_spike, free_spike], axis=1)
    spike_length = jax.random.uniform(random_subkeys[11], (ATTENTION_HEADS, 2), minval=0.22, maxval=0.5)
    spike_hits = (jnp.arange(SEQUENCE_TOKENS)[:, None, None] == spike_position[None]).astype(jnp.float32)
    spike_events = -jnp.sum(spike_hits * spike_length[None], axis=2)
    return (steady_decay + spike_events[:, :, None]).reshape(SEQUENCE_TOKENS, ATTENTION_HEADS * KEY_CHANNELS).astype(jnp.float32)


def draw_fwd_decay(key, part):
    return decay_law(key, 23)


def draw_bwd_decay(key, part):
    return decay_law(key, 37)


def strengthened(values, rng, source, target, blocks, factor):
    def block_of(dim):
        return (jnp.arange(values.shape[dim]) // (values.shape[dim] // blocks)).reshape((-1,) + (1,) * (values.ndim - 1 - dim))

    near = jax.random.permutation(rng, blocks)[block_of(target)]
    second = (block_of(target) + blocks // 2) % blocks
    return jnp.where((block_of(source) == near) | (block_of(source) == second), factor * values, values)


def shard_levels(rng, extent, cuts, least, largest):
    def one(axis_at, parts):
        heights = jax.random.uniform(jax.random.fold_in(jax.random.fold_in(rng, 6), axis_at), (parts,), jnp.float32, least / len(cuts), largest / len(cuts))
        return jnp.repeat(jnp.exp(heights), extent[axis_at] // parts).reshape((-1,) + (1,) * (len(extent) - axis_at - 1))

    gain = one(*cuts[0])
    for cut in cuts[1:]:
        gain = gain * one(*cut)
    return gain


def gaussian(stream_key, extent, deviation, limit, cuts=(), kind=jnp.bfloat16):
    result = jax.random.normal(stream_key, extent, jnp.float32) * deviation
    if len(cuts) > 0:
        result = shard_levels(stream_key, extent, cuts, -0.22, 0.18) * result
    return jnp.clip(result, min=-limit, max=limit).astype(kind)


def gaussian_with(own_key, shape, width, bound, cuts, heavy, kind=jnp.bfloat16):
    values = width * jax.random.normal(own_key, shape, jnp.float32)
    if cuts:
        values = values * shard_levels(own_key, shape, cuts, -0.22, 0.18)
    return jnp.clip(strengthened(values, jax.random.fold_in(own_key, 3), *heavy), -bound, bound).astype(kind)


def setup_inputs(seed: int = 0) -> dict:
    key_list = jax.random.split(jax.random.key(seed), 14)
    layer_grad = gaussian_with(key_list[0], (SEQUENCE_TOKENS, D), 1.0, 6.0, ((0, 8),), (0, 1, 8, 2.0))
    routes = draw_routes(jax.random.fold_in(key_list[13], 71), 0)
    route_weight = jnp.clip(0.1 + 0.79999997 * jax.random.uniform(key_list[2], (SEQUENCE_TOKENS, 2), jnp.float32) ** shard_levels(key_list[2], (SEQUENCE_TOKENS, 2), ((0, 8),), -0.2, 0.2), 0.1, 0.9)
    slot_tokens = gaussian(key_list[3], (EXPERTS, SLOTS, D), 1.0, 6.0, ((0, 8),))
    gate_proj = gaussian(key_list[4], (EXPERTS, D, FF), D ** -0.5, 0.125, ((0, 8), (2, 4)))
    up_proj = gaussian(key_list[5], (EXPERTS, D, FF), D ** -0.5, 0.125, ((0, 8), (2, 4)))
    down_proj = gaussian(key_list[6], (EXPERTS, FF, D), FF ** -0.5, 0.1875, ((0, 8), (1, 4)))
    out_proj = gaussian(key_list[7], (D, ATTENTION_HEADS * DV), (ATTENTION_HEADS * DV) ** -0.5, 0.1875, ((1, 4),))
    queries = gaussian(key_list[8], (SEQUENCE_TOKENS, ATTENTION_HEADS * KEY_CHANNELS), 1.0, 6.0, ((0, 8), (1, 4)))
    keys = gaussian(key_list[9], (SEQUENCE_TOKENS, ATTENTION_HEADS * KEY_CHANNELS), 1.0, 6.0, ((0, 8), (1, 4)))
    values = gaussian(key_list[10], (SEQUENCE_TOKENS, ATTENTION_HEADS * DV), 1.0, 6.0, ((0, 8), (1, 4)))
    fwd_decay = draw_fwd_decay(jax.random.fold_in(key_list[13], 71), 0)
    bwd_decay = draw_bwd_decay(jax.random.fold_in(key_list[13], 71), 0)
    return {"layer_grad": layer_grad, "routes": routes, "route_weight": route_weight, "slot_tokens": slot_tokens, "gate_proj": gate_proj, "up_proj": up_proj, "down_proj": down_proj, "out_proj": out_proj, "queries": queries, "keys": keys, "values": values, "fwd_decay": fwd_decay, "bwd_decay": bwd_decay}


EPSILON = 1e-06

def sweep(query_rows, keyrows, valrows, log_decay, strict):
    nheads, length, kwidth = query_rows.shape
    vwidth = valrows.shape[-1]
    number = length // BLOCK
    offset = -1 if strict else 0
    causal = jnp.tril(jnp.ones((BLOCK, BLOCK), jnp.float32), offset)

    def split(array):
        return jnp.moveaxis(array.reshape(nheads, number, BLOCK, array.shape[-1]), 1, 0)

    def advance(carried_state, pieces):
        query_block, key_block, value_block, gblock = pieces
        running_total = jnp.cumsum(gblock, axis=1)
        middle = running_total[:, BLOCK // 2 - 1:BLOCK // 2, :]
        scores = jnp.einsum('hik,hjk->hij', query_block * jnp.exp(running_total - middle), key_block * jnp.exp(middle - running_total), precision=lax.Precision.HIGHEST) * causal
        inner = jnp.einsum('hij,hjv->hiv', scores, value_block, precision=lax.Precision.HIGHEST)
        outer_product = jnp.einsum('zuw,zwo->zuo', query_block * jnp.exp(running_total), carried_state, precision=lax.Precision.HIGHEST)
        final_row = running_total[:, -1:, :]
        fresh_state = jnp.einsum('xor,xot->xrt', key_block * jnp.exp(final_row - running_total), value_block, precision=lax.Precision.HIGHEST)
        return (jnp.exp(final_row[:, 0, :])[:, :, None] * carried_state + fresh_state, inner + outer_product)
    start_state = jnp.zeros((nheads, kwidth, vwidth), jnp.float32)
    final, outputs = lax.scan(advance, start_state, (split(query_rows), split(keyrows), split(valrows), split(log_decay)))
    return (jnp.moveaxis(outputs, 0, 1).reshape(nheads, length, vwidth), final)

def slot_ranks(expert_ids, experts):
    members = (expert_ids[:, None] == jnp.arange(experts, dtype=jnp.int32)[None, :]).astype(jnp.int32)
    before = jnp.cumsum(members, axis=0) - members
    return lax.optimization_barrier(jnp.sum(before * members, axis=1))

def mixer_forward(query_rows, keyrows, valrows, fwd_log, bwd_log):
    forward_out, forward_end = sweep(query_rows, keyrows, valrows, fwd_log, False)
    backward_out, backward_end = sweep(jnp.flip(query_rows, 1), jnp.flip(keyrows, 1), jnp.flip(valrows, 1), jnp.flip(bwd_log, 1), True)
    mixed = forward_out + jnp.flip(backward_out, 1)
    return mixed * lax.rsqrt(lax.optimization_barrier(jnp.mean(mixed * mixed, axis=-1, keepdims=True)) + EPSILON)

def expert_back(pieces):
    inputs, inbound, w_gate, w_up, w_down = pieces
    gate = jnp.dot(inputs, w_gate, preferred_element_type=jnp.float32)
    upper = jnp.dot(inputs, w_up, preferred_element_type=jnp.float32)
    sigma = jax.nn.sigmoid(gate)
    act = (gate * sigma * upper).astype(jnp.bfloat16)
    grad_down = lax.dot_general(act, inbound, (((0,), (0,)), ((), ())), preferred_element_type=jnp.float32)
    act_grad = lax.dot_general(inbound, w_down, (((1,), (1,)), ((), ())), preferred_element_type=jnp.float32)
    up_delta = (act_grad * gate * sigma).astype(jnp.bfloat16)
    gate_delta = (act_grad * upper * sigma * (1.0 + gate * (1.0 - sigma))).astype(jnp.bfloat16)
    grad_gate = lax.dot_general(inputs, gate_delta, (((0,), (0,)), ((), ())), preferred_element_type=jnp.float32)
    grad_up = lax.dot_general(inputs, up_delta, (((0,), (0,)), ((), ())), preferred_element_type=jnp.float32)
    share = w_gate.shape[1] // N_TP
    total = jnp.zeros((inputs.shape[0], inputs.shape[1]), jnp.float32)
    for portion in range(N_TP):
        lower_col = portion * share
        partial_sum = lax.dot_general(gate_delta[:, lower_col:lower_col + share], w_gate[:, lower_col:lower_col + share], (((1,), (1,)), ((), ())), preferred_element_type=jnp.float32)
        partial_sum = partial_sum + lax.dot_general(up_delta[:, lower_col:lower_col + share], w_up[:, lower_col:lower_col + share], (((1,), (1,)), ((), ())), preferred_element_type=jnp.float32)
        total = total + lax.optimization_barrier(partial_sum.astype(jnp.bfloat16)).astype(jnp.float32)
    return (grad_gate.astype(jnp.bfloat16), grad_up.astype(jnp.bfloat16), grad_down.astype(jnp.bfloat16), total.astype(jnp.bfloat16))

def reference(layer_grad, routes, route_weight, slot_tokens, gate_proj, up_proj, down_proj, out_proj, queries, keys, values, fwd_decay, bwd_decay):
    per_block = routes.reshape(N_SP, TOK_DEV * 2).astype(jnp.int32)
    ranks = jax.vmap(functools.partial(slot_ranks, experts=EXPERTS))(per_block)
    source = jnp.arange(N_SP, dtype=jnp.int32)[:, None]
    kept = ranks < CAP
    target = jnp.where(kept, per_block * SLOTS + source * CAP + ranks, EXPERTS * SLOTS).reshape(-1).astype(jnp.int32)
    weighted = (layer_grad.astype(jnp.float32)[:, None, :] * route_weight[:, :, None]).astype(jnp.bfloat16).reshape(SEQUENCE_TOKENS * 2, D)
    inbound = jnp.zeros((EXPERTS * SLOTS + 1, D), jnp.bfloat16).at[target].set(weighted)[:EXPERTS * SLOTS].reshape(EXPERTS, SLOTS, D)
    grad_gate, grad_up, grad_down, slot_grad = lax.map(expert_back, (slot_tokens, inbound, gate_proj, up_proj, down_proj))
    picked = slot_grad.reshape(EXPERTS * SLOTS, D)[jnp.minimum(target, EXPERTS * SLOTS - 1)]
    picked = picked.astype(jnp.float32) * kept.reshape(-1, 1).astype(jnp.float32)
    moe_grad = lax.optimization_barrier(jnp.sum(picked.reshape(SEQUENCE_TOKENS, 2, D), axis=1))
    stream_grad = (layer_grad.astype(jnp.float32) + moe_grad).astype(jnp.bfloat16)
    scale = KEY_CHANNELS ** (-0.5)

    def split_heads(array, size):
        return array.astype(jnp.float32).reshape(SEQUENCE_TOKENS, ATTENTION_HEADS, size).transpose(1, 0, 2)

    def merge_heads(array):
        return array.transpose(1, 0, 2).reshape(SEQUENCE_TOKENS, -1)
    mixed, pullback = jax.vjp(mixer_forward, split_heads(queries, KEY_CHANNELS) * scale, split_heads(keys, KEY_CHANNELS), split_heads(values, DV), split_heads(fwd_decay, KEY_CHANNELS), split_heads(bwd_decay, KEY_CHANNELS))
    mixed_rows = merge_heads(mixed).astype(jnp.bfloat16)
    proj_grad = lax.dot_general(stream_grad, mixed_rows, (((0,), (0,)), ((), ())), preferred_element_type=jnp.float32)
    mixed_grad = jnp.dot(stream_grad, out_proj, preferred_element_type=jnp.float32)
    query_part, key_part, value_part, fwd_part, bwd_part = pullback(split_heads(mixed_grad, DV))
    return (grad_gate, grad_up, grad_down, proj_grad, (merge_heads(query_part) * scale).astype(jnp.bfloat16), merge_heads(key_part).astype(jnp.bfloat16), merge_heads(value_part).astype(jnp.bfloat16))
```

```python
import functools

import jax
import jax.numpy as jnp
from jax import lax
from jax.experimental import pallas as pl
from jax.experimental.pallas import tpu as pltpu
from jax.sharding import PartitionSpec as P

KEY_CHANNELS = 64
DV = 128
BLOCK = 64
EPSILON = 1e-06
SCALE = KEY_CHANNELS ** (-0.5)
TAIL = 16
F32 = jnp.float32
BF16 = jnp.bfloat16
HIGHEST = lax.Precision.HIGHEST


def mm(a, b, contract, precision=None):
    return lax.dot_general(
        a, b, ((contract[:1], contract[1:]), ((), ())), preferred_element_type=F32, precision=precision
    )


def bmm(a, b, contract):
    return mm(a.astype(BF16), b.astype(BF16), contract)


def call(kernel, outs, cost, *args, **scratch):
    flops, nbytes = cost
    return pl.pallas_call(
        kernel,
        out_shape=outs,
        in_specs=[pl.BlockSpec(memory_space=pltpu.VMEM)] * len(args),
        out_specs=jax.tree.map(lambda _: pl.BlockSpec(memory_space=pltpu.VMEM), outs),
        cost_estimate=pl.CostEstimate(flops=flops, bytes_accessed=nbytes, transcendentals=0),
        **scratch,
    )(*args)


def iota(shape, dim):
    return lax.broadcasted_iota(jnp.int32, shape, dim)


def cumulative(fwd_ref, bwd_ref):
    length = fwd_ref.shape[0]
    row, col = iota((length, length), 0), iota((length, length), 1)
    rising = mm((col <= row).astype(F32), fwd_ref[...], (1, 0), HIGHEST)
    falling = mm((col >= row).astype(F32), bwd_ref[...], (1, 0), HIGHEST)
    return rising, falling


def head_mask(h, shape):
    return (iota(shape, 1) // KEY_CHANNELS) == h


def masked(h, array):
    return jnp.where(head_mask(h, array.shape), array, jnp.zeros_like(array))


def put_chunks(out_ref, fwd_state, bwd_state, fwd_total, bwd_total, forward_up):
    n = out_ref.shape[0]
    me = lax.axis_index("sp")
    lanes = out_ref.shape[2]

    def packed(state, total):
        hi = total.astype(BF16)
        rest = total - hi.astype(F32)
        mid = rest.astype(BF16)
        low = (rest - mid.astype(F32)).astype(BF16)
        row = iota((TAIL, lanes), 0)
        wide = lambda a: jnp.broadcast_to(a.astype(F32), (TAIL, lanes))
        tail = jnp.where(
            row == 0, wide(hi), jnp.where(row == 1, wide(mid), jnp.where(row == 2, wide(low), 0.0))
        )
        return state, tail

    fstate, ftail = packed(fwd_state, fwd_total)
    bstate, btail = packed(bwd_state, bwd_total)

    def one(d, carry):
        up = (d > me) if forward_up else (d < me)
        out_ref[pl.ds(d, 1), 0:DV, :] = jnp.where(up, fstate, bstate).astype(BF16)[None]
        out_ref[pl.ds(d, 1), DV : DV + TAIL, :] = jnp.where(up, ftail, btail).astype(BF16)[None]
        return carry

    lax.fori_loop(0, n, one, 0)


def take_chunks(in_ref):
    n, _, lanes = in_ref.shape
    me = lax.axis_index("sp")

    def piece(s):
        state = in_ref[pl.ds(s, 1), 0:DV, :][0].astype(F32)
        tail = in_ref[pl.ds(s, 1), DV : DV + TAIL, :][0].astype(F32)
        total = tail[0:1] + tail[1:2] + tail[2:3]
        return state, jnp.exp(total)

    def ahead(s, state):
        fresh, decay = piece(s)
        return jnp.where(s < me, state * decay + fresh, state)

    def behind(hop, state):
        s = n - 1 - hop
        fresh, decay = piece(s)
        return jnp.where(s > me, state * decay + fresh, state)

    zero = jnp.zeros((DV, lanes), F32)
    return lax.fori_loop(0, n, ahead, zero), lax.fori_loop(0, n, behind, zero)


def dispatch_kernel(routes_ref, weight_ref, grad_ref, out_ref, spread_ref, own_ref, *, experts, capacity):
    rows = routes_ref.shape[0]
    share = own_ref.shape[1]
    slots = experts * capacity
    wide = max(128, experts)
    tp = lax.axis_index("tp")
    lane = iota((rows, wide), 1)
    first = routes_ref[:, 0:1]
    second = routes_ref[:, 1:2]
    is_first = lane == first
    is_second = lane == second
    members = jnp.where(is_first, 1.0, 0.0) + jnp.where(is_second, 1.0, 0.0)
    row, col = iota((rows, rows), 0), iota((rows, rows), 1)
    before = bmm((col < row).astype(F32), members, (1, 0))
    slot = iota((rows, slots), 1)

    def spread(chosen, mine):
        rank = jnp.sum(jnp.where(mine, before, 0.0), axis=1, keepdims=True).astype(jnp.int32)
        target = jnp.where(rank < capacity, chosen * capacity + rank, -1)
        return jnp.where(slot == target, 1.0, 0.0)

    one = spread(first, is_first)
    two = spread(second, is_second)
    own = grad_ref[:, pl.ds(pl.multiple_of(tp * share, 128), share)]
    own_ref[...] = own
    wide_own = own.astype(F32)
    left = (wide_own * weight_ref[:, 0:1]).astype(BF16)
    right = (wide_own * weight_ref[:, 1:2]).astype(BF16)
    out_ref[...] = (bmm(one, left, (0, 0)) + bmm(two, right, (0, 0))).astype(BF16)
    spread_ref[...] = (one + two).astype(BF16)


def ends_kernel(k_ref, v_ref, fwd_ref, bwd_ref, out_ref):
    length, lanes = k_ref.shape
    rising, falling = cumulative(fwd_ref, bwd_ref)
    fwd_total = rising[length - 1 : length]
    bwd_total = falling[0:1]
    k = k_ref[...].astype(F32)
    kf = k * jnp.exp(fwd_total - rising)
    kb = k * jnp.exp(bwd_total - falling)
    fend = jnp.zeros((DV, lanes), F32)
    bend = jnp.zeros((DV, lanes), F32)
    for h in range(lanes // KEY_CHANNELS):
        v = v_ref[:, h * DV : (h + 1) * DV]
        fend = fend + bmm(v, masked(h, kf), (0, 0))
        bend = bend + bmm(v, masked(h, kb), (0, 0))
    put_chunks(out_ref, fend, bend, fwd_total, bwd_total, True)


def block_factors(b, rising, falling):
    s = b * BLOCK
    fmid = rising[s + BLOCK // 2 - 1 : s + BLOCK // 2]
    bmid = falling[s + BLOCK // 2 : s + BLOCK // 2 + 1]
    block = slice(s, s + BLOCK)
    return (
        jnp.exp(rising[block] - fmid),
        jnp.exp(jnp.minimum(fmid - rising, 64.0)),
        jnp.exp(falling[block] - bmid),
        jnp.exp(jnp.minimum(bmid - falling, 64.0)),
    )


def causal(b, length):
    return iota((BLOCK, length), 1) <= iota((BLOCK, length), 0) + b * BLOCK


def forward_kernel(in_ref, q_ref, k_ref, v_ref, fwd_ref, bwd_ref, score_ref, o_ref, rows_ref, s_ref, r_ref):
    length, lanes = q_ref.shape
    heads = lanes // KEY_CHANNELS
    entry, back_entry = take_chunks(in_ref)
    s_ref[...] = entry
    r_ref[...] = back_entry
    rising, falling = cumulative(fwd_ref, bwd_ref)
    q = q_ref[...].astype(F32) * SCALE
    k = k_ref[...].astype(F32)
    for b in range(length // BLOCK):
        block = slice(b * BLOCK, (b + 1) * BLOCK)
        fq, fk, bq, bk = block_factors(b, rising, falling)
        qf = q[block] * fq
        qb = q[block] * bq
        kf = (k * fk).astype(BF16)
        kb = (k * bk).astype(BF16)
        keep = causal(b, length)
        for h in range(heads):
            fs = bmm(masked(h, qf), kf, (1, 1))
            bs = bmm(masked(h, qb), kb, (1, 1))
            score_ref[h, block, :] = jnp.where(keep, fs, bs).astype(BF16)
    qs = q * jnp.exp(rising)
    qr = q * jnp.exp(falling)
    for h in range(heads):
        cols = slice(h * DV, (h + 1) * DV)
        o = mm(score_ref[h], v_ref[:, cols], (1, 0))
        o = o + bmm(masked(h, qs), entry, (1, 1)) + bmm(masked(h, qr), back_entry, (1, 1))
        o_ref[:, cols] = o
        rms = lax.rsqrt(jnp.mean(o * o, axis=1, keepdims=True) + EPSILON)
        rows_ref[:, cols] = (o * rms).astype(BF16)


def cotangent_kernel(*refs, parts):
    streams = refs[:parts]
    proj_ref, o_ref, q_ref, fwd_ref, bwd_ref, do_ref, out_ref = refs[parts:]
    length, lanes = q_ref.shape
    share = streams[0].shape[1]
    tp = lax.axis_index("tp")
    grad = jnp.zeros(o_ref.shape, F32)
    for m in range(parts):
        first = pl.multiple_of((tp ^ m) * share, 128)
        grad = grad + mm(streams[m][...], proj_ref[pl.ds(first, share), :], (1, 0))
    rising, falling = cumulative(fwd_ref, bwd_ref)
    q = q_ref[...].astype(F32) * SCALE
    qs = q * jnp.exp(rising)
    qr = q * jnp.exp(falling)
    ds = jnp.zeros((DV, lanes), F32)
    dr = jnp.zeros((DV, lanes), F32)
    for h in range(lanes // KEY_CHANNELS):
        cols = slice(h * DV, (h + 1) * DV)
        o = o_ref[:, cols]
        rms = lax.rsqrt(jnp.mean(o * o, axis=1, keepdims=True) + EPSILON)
        mixed = o * rms
        dm = grad[:, cols]
        do = (rms * (dm - mixed * jnp.mean(dm * mixed, axis=1, keepdims=True))).astype(BF16)
        do_ref[:, cols] = do
        ds = ds + bmm(do, masked(h, qs), (0, 0))
        dr = dr + bmm(do, masked(h, qr), (0, 0))
    put_chunks(out_ref, ds, dr, rising[length - 1 : length], falling[0:1], False)


def proj_kernel(*refs, parts):
    streams = refs[:parts]
    rows_ref, out_ref = refs[parts:]
    share = streams[0].shape[1]
    tp = lax.axis_index("tp")
    for m in range(parts):
        first = pl.multiple_of((tp ^ m) * share, 128)
        out_ref[pl.ds(first, share), :] = mm(streams[m][...], rows_ref[...], (0, 0)).astype(BF16)


def local_kernel(do_ref, score_ref, q_ref, k_ref, v_ref, fwd_ref, bwd_ref, s_ref, r_ref, dq_ref, dk_ref, dv_ref):
    length, lanes = q_ref.shape
    heads = lanes // KEY_CHANNELS
    rising, falling = cumulative(fwd_ref, bwd_ref)
    q = q_ref[...].astype(F32) * SCALE
    k = k_ref[...].astype(F32)
    dk = jnp.zeros((length, lanes), F32)
    reach = jnp.zeros((length, lanes), F32)
    reach_back = jnp.zeros((length, lanes), F32)
    for h in range(heads):
        cols = slice(h * DV, (h + 1) * DV)
        do = do_ref[:, cols]
        dv_ref[:, cols] = mm(score_ref[h], do, (0, 0))
        reach = reach + bmm(do, masked(h, s_ref[...]), (1, 0))
        reach_back = reach_back + bmm(do, masked(h, r_ref[...]), (1, 0))
    far = reach * jnp.exp(rising) + reach_back * jnp.exp(falling)
    for b in range(length // BLOCK):
        block = slice(b * BLOCK, (b + 1) * BLOCK)
        fq, fk, bq, bk = block_factors(b, rising, falling)
        qf = q[block] * fq
        qb = q[block] * bq
        kf = k * fk
        kb = k * bk
        keep = causal(b, length)
        dqf = jnp.zeros((BLOCK, lanes), F32)
        dqb = jnp.zeros((BLOCK, lanes), F32)
        dkf = jnp.zeros((length, lanes), F32)
        dkb = jnp.zeros((length, lanes), F32)
        for h in range(heads):
            cols = slice(h * DV, (h + 1) * DV)
            dscore = mm(do_ref[block, cols], v_ref[:, cols], (1, 1))
            df = jnp.where(keep, dscore, 0.0).astype(BF16)
            db = jnp.where(keep, 0.0, dscore).astype(BF16)
            dqf = dqf + bmm(df, masked(h, kf), (1, 0))
            dqb = dqb + bmm(db, masked(h, kb), (1, 0))
            dkf = dkf + bmm(df, masked(h, qf), (0, 0))
            dkb = dkb + bmm(db, masked(h, qb), (0, 0))
        dq_ref[block, :] = ((dqf * fq + dqb * bq + far[block]) * SCALE).astype(BF16)
        dk = dk + dkf * fk + dkb * bk
    dk_ref[...] = dk


def last_kernel(in_ref, k_ref, v_ref, fwd_ref, bwd_ref, dk_in, dv_in, dk_ref, dv_ref):
    length, lanes = k_ref.shape
    earlier, later = take_chunks(in_ref)
    rising, falling = cumulative(fwd_ref, bwd_ref)
    ff = jnp.exp(rising[length - 1 : length] - rising)
    bf = jnp.exp(falling[0:1] - falling)
    k = k_ref[...].astype(F32)
    kf = k * ff
    kb = k * bf
    ahead = jnp.zeros((length, lanes), F32)
    behind = jnp.zeros((length, lanes), F32)
    for h in range(lanes // KEY_CHANNELS):
        cols = slice(h * DV, (h + 1) * DV)
        v = v_ref[:, cols]
        ahead = ahead + bmm(v, masked(h, later), (1, 0))
        behind = behind + bmm(v, masked(h, earlier), (1, 0))
        dv = dv_in[:, cols] + bmm(masked(h, kf), later, (1, 1)) + bmm(masked(h, kb), earlier, (1, 1))
        dv_ref[:, cols] = dv.astype(BF16)
    dk_ref[...] = (dk_in[...] + ahead * ff + behind * bf).astype(BF16)


def exchange(array):
    return lax.all_to_all(array, "sp", split_axis=0, concat_axis=0, tiled=True)


def on_device(
    layer_grad,
    routes,
    route_weight,
    slot_tokens,
    gate_proj,
    up_proj,
    down_proj,
    out_proj,
    queries,
    keys,
    values,
    fwd_decay,
    bwd_decay,
):
    sds = jax.ShapeDtypeStruct
    devices = lax.axis_size("sp")
    parts = lax.axis_size("tp")
    tp = lax.axis_index("tp")
    rows, width = layer_grad.shape
    slots = slot_tokens.shape[1]
    capacity = slots // devices
    share = width // parts
    lanes = keys.shape[1]
    heads = lanes // KEY_CHANNELS
    vwidth = values.shape[1]

    def swap(array, bit):
        return lax.ppermute(array, "tp", [(i, i ^ bit) for i in range(parts)])

    def gather_parts(own):
        pieces = {0: own}
        bit = parts // 2
        while bit:
            for m in list(pieces):
                pieces[m ^ bit] = swap(pieces[m], bit)
            bit //= 2
        return [pieces[m] for m in range(parts)]

    outgoing, spread, own_grad = call(
        functools.partial(dispatch_kernel, experts=devices, capacity=capacity),
        (sds((slots, share), BF16), sds((rows, slots), BF16), sds((rows, share), BF16)),
        (8 * rows * slots * share, 3 << 20),
        routes,
        route_weight,
        layer_grad,
    )
    arrived = exchange(outgoing.reshape(devices, capacity, share)).reshape(slots, share)

    chunk = sds((devices, DV + TAIL, lanes), BF16)
    ends = call(ends_kernel, chunk, (2 * 10**9, 3 << 20), keys, values, fwd_decay, bwd_decay)
    inbound = gather_parts(arrived)
    states = exchange(ends)

    x = slot_tokens[0]
    w_gate, w_up, w_down = gate_proj[0], up_proj[0], down_proj[0]
    gate = jnp.dot(x, w_gate, preferred_element_type=F32)
    upper = jnp.dot(x, w_up, preferred_element_type=F32)
    sigma = jax.nn.sigmoid(gate)
    act = (gate * sigma * upper).astype(BF16)

    scores, o, mixed_rows, entry, back_entry = call(
        forward_kernel,
        (
            sds((heads, rows, rows), BF16),
            sds((rows, vwidth), F32),
            sds((rows, vwidth), BF16),
            sds((DV, lanes), F32),
            sds((DV, lanes), F32),
        ),
        (4 * 10**9, 3 << 20),
        states,
        queries,
        keys,
        values,
        fwd_decay,
        bwd_decay,
    )

    act_grad = 0.0
    for m in range(parts):
        w = lax.dynamic_slice_in_dim(w_down, (tp ^ m) * share, share, 1)
        act_grad = act_grad + mm(inbound[m], w, (1, 1))
    up_delta = (act_grad * gate * sigma).astype(BF16)
    gate_delta = (act_grad * upper * sigma * (1.0 + gate * (1.0 - sigma))).astype(BF16)

    def slot_piece(m):
        wg = lax.dynamic_slice_in_dim(w_gate, (tp ^ m) * share, share, 0)
        wu = lax.dynamic_slice_in_dim(w_up, (tp ^ m) * share, share, 0)
        return (mm(gate_delta, wg, (1, 1)) + mm(up_delta, wu, (1, 1))).astype(BF16)

    pieces = {m: slot_piece(m) for m in reversed(range(parts))}
    bit = 1
    while bit < parts:
        kept = [m for m in pieces if not m & bit]
        pieces = {
            m: (pieces[m].astype(F32) + swap(pieces[m ^ bit], bit).astype(F32)).astype(BF16)
            for m in kept
        }
        bit *= 2
    back = exchange(pieces[0].reshape(devices, capacity, share)).reshape(slots, share)

    grad_gate = mm(x, gate_delta, (0, 0)).astype(BF16)
    grad_up = mm(x, up_delta, (0, 0)).astype(BF16)
    grad_down = jnp.zeros(w_down.shape, BF16)
    for m in range(parts):
        grad_down = lax.dynamic_update_slice_in_dim(
            grad_down, mm(act, inbound[m], (0, 0)).astype(BF16), (tp ^ m) * share, 1
        )

    stream = (own_grad.astype(F32) + mm(spread, back, (1, 0))).astype(BF16)
    streams = gather_parts(stream)
    do, cots = call(
        functools.partial(cotangent_kernel, parts=parts),
        (sds((rows, vwidth), BF16), chunk),
        (2 * 10**9, 4 << 20),
        *streams,
        out_proj,
        o,
        queries,
        fwd_decay,
        bwd_decay,
    )
    cots = exchange(cots)
    term = call(
        functools.partial(proj_kernel, parts=parts),
        sds((width, vwidth), BF16),
        (2 * 10**9, 2 << 20),
        *streams,
        mixed_rows,
    )
    terms = exchange(term.reshape(devices, width // devices, vwidth))
    dq, dk_near, dv_near = call(
        local_kernel,
        (sds((rows, lanes), BF16), sds((rows, lanes), F32), sds((rows, vwidth), F32)),
        (4 * 10**9, 3 << 20),
        do,
        scores,
        queries,
        keys,
        values,
        fwd_decay,
        bwd_decay,
        entry,
        back_entry,
    )
    dk, dv = call(
        last_kernel,
        (sds((rows, lanes), BF16), sds((rows, vwidth), BF16)),
        (2 * 10**9, 3 << 20),
        cots,
        keys,
        values,
        fwd_decay,
        bwd_decay,
        dk_near,
        dv_near,
    )
    proj_grad = jnp.sum(terms.astype(F32), axis=0)
    return (grad_gate[None], grad_up[None], grad_down[None], proj_grad, dq, dk, dv)


def solution(mesh):
    placed = (
        P("sp", None),
        P("sp", None),
        P("sp", None),
        P("sp", None, None),
        P("sp", None, "tp"),
        P("sp", None, "tp"),
        P("sp", "tp", None),
        P(None, "tp"),
        P("sp", "tp"),
        P("sp", "tp"),
        P("sp", "tp"),
        P("sp", "tp"),
        P("sp", "tp"),
    )
    return jax.shard_map(
        on_device,
        mesh=mesh,
        in_specs=placed,
        out_specs=(
            P("sp", None, "tp"),
            P("sp", None, "tp"),
            P("sp", "tp", None),
            P("sp", "tp"),
            P("sp", "tp"),
            P("sp", "tp"),
            P("sp", "tp"),
        ),
        check_vma=False,
    )
```

```python
import functools

import jax
import jax.numpy as jnp
from jax import lax
from jax.experimental import pallas as pl
from jax.experimental.pallas import tpu as pltpu
from jax.sharding import PartitionSpec as P

KEY_CHANNELS = 64
DV = 128
BLOCK = 64
EPSILON = 1e-06
SCALE = KEY_CHANNELS ** (-0.5)
TAIL = 16
F32 = jnp.float32
BF16 = jnp.bfloat16
HIGHEST = lax.Precision.HIGHEST


def mm(a, b, contract, precision=None):
    return lax.dot_general(
        a, b, ((contract[:1], contract[1:]), ((), ())), preferred_element_type=F32, precision=precision
    )


def bmm(a, b, contract):
    return mm(a.astype(BF16), b.astype(BF16), contract)


def call(kernel, outs, cost, *args, **scratch):
    flops, nbytes = cost
    return pl.pallas_call(
        kernel,
        out_shape=outs,
        in_specs=[pl.BlockSpec(memory_space=pltpu.VMEM)] * len(args),
        out_specs=jax.tree.map(lambda _: pl.BlockSpec(memory_space=pltpu.VMEM), outs),
        cost_estimate=pl.CostEstimate(flops=flops, bytes_accessed=nbytes, transcendentals=0),
        **scratch,
    )(*args)


def iota(shape, dim):
    return lax.broadcasted_iota(jnp.int32, shape, dim)


def cumulative(fwd_ref, bwd_ref):
    length = fwd_ref.shape[0]
    row, col = iota((length, length), 0), iota((length, length), 1)
    rising = mm((col <= row).astype(F32), fwd_ref[...], (1, 0), HIGHEST)
    falling = mm((col >= row).astype(F32), bwd_ref[...], (1, 0), HIGHEST)
    return rising, falling


def head_mask(h, shape):
    return (iota(shape, 1) // KEY_CHANNELS) == h


def masked(h, array):
    return jnp.where(head_mask(h, array.shape), array, jnp.zeros_like(array))


def put_chunks(out_ref, fwd_state, bwd_state, fwd_total, bwd_total, forward_up):
    n = out_ref.shape[0]
    me = lax.axis_index("sp")
    lanes = out_ref.shape[2]

    def packed(state, total):
        hi = total.astype(BF16)
        rest = total - hi.astype(F32)
        mid = rest.astype(BF16)
        low = (rest - mid.astype(F32)).astype(BF16)
        row = iota((TAIL, lanes), 0)
        wide = lambda a: jnp.broadcast_to(a.astype(F32), (TAIL, lanes))
        tail = jnp.where(
            row == 0, wide(hi), jnp.where(row == 1, wide(mid), jnp.where(row == 2, wide(low), 0.0))
        )
        return state, tail

    fstate, ftail = packed(fwd_state, fwd_total)
    bstate, btail = packed(bwd_state, bwd_total)

    def one(d, carry):
        up = (d > me) if forward_up else (d < me)
        out_ref[pl.ds(d, 1), 0:DV, :] = jnp.where(up, fstate, bstate).astype(BF16)[None]
        out_ref[pl.ds(d, 1), DV : DV + TAIL, :] = jnp.where(up, ftail, btail).astype(BF16)[None]
        return carry

    lax.fori_loop(0, n, one, 0)


def take_chunks(in_ref):
    n, _, lanes = in_ref.shape
    me = lax.axis_index("sp")

    def piece(s):
        state = in_ref[pl.ds(s, 1), 0:DV, :][0].astype(F32)
        tail = in_ref[pl.ds(s, 1), DV : DV + TAIL, :][0].astype(F32)
        total = tail[0:1] + tail[1:2] + tail[2:3]
        return state, jnp.exp(total)

    def ahead(s, state):
        fresh, decay = piece(s)
        return jnp.where(s < me, state * decay + fresh, state)

    def behind(hop, state):
        s = n - 1 - hop
        fresh, decay = piece(s)
        return jnp.where(s > me, state * decay + fresh, state)

    zero = jnp.zeros((DV, lanes), F32)
    return lax.fori_loop(0, n, ahead, zero), lax.fori_loop(0, n, behind, zero)


def peers(n):
    me = lax.axis_index("sp")
    return me, [lax.rem(me + hop, n) for hop in range(1, n)]


def greet(n):
    _, others = peers(n)
    barrier = pltpu.get_barrier_semaphore()
    for other in others:
        pl.semaphore_signal(
            barrier, inc=1, device_id={"sp": other}, device_id_type=pl.DeviceIdType.MESH
        )
    pl.semaphore_wait(barrier, n - 1)


def send_all(n, source, landing, send_sem, recv_sem):
    me, others = peers(n)
    copies = []
    for hop, other in enumerate(others):
        copy = pltpu.make_async_remote_copy(
            src_ref=source.at[other],
            dst_ref=landing.at[me],
            send_sem=send_sem.at[hop],
            recv_sem=recv_sem.at[hop],
            device_id={"sp": other},
            device_id_type=pl.DeviceIdType.MESH,
        )
        copy.start()
        copies.append(copy)
    return copies


def keep_own(source, landing):
    me = lax.axis_index("sp")
    landing[pl.ds(me, 1)] = source[pl.ds(me, 1)]


def exchange_kernel(*refs, arrays):
    sources, landings, sems = refs[:arrays], refs[arrays : 2 * arrays], refs[2 * arrays :]
    n = sources[0].shape[0]
    greet(n)
    copies = []
    for i in range(arrays):
        copies += send_all(n, sources[i], landings[i], sems[2 * i], sems[2 * i + 1])
    for source, landing in zip(sources, landings):
        keep_own(source, landing)
    for copy in copies:
        copy.wait()


def sems(n, arrays):
    return [pltpu.SemaphoreType.DMA((n - 1,)) for _ in range(2 * arrays)]


def send_params(number):
    return pltpu.CompilerParams(collective_id=number, has_side_effects=True)


def exchange_many(number, *arrays):
    n = arrays[0].shape[0]
    return call(
        functools.partial(exchange_kernel, arrays=len(arrays)),
        tuple(jax.ShapeDtypeStruct(a.shape, a.dtype) for a in arrays),
        (2 * 10**9, 8 << 20),
        *arrays,
        scratch_shapes=sems(n, len(arrays)),
        compiler_params=send_params(number),
    )


def dispatch_kernel(routes_ref, weight_ref, grad_ref, out_ref, spread_ref, own_ref, *, experts, capacity):
    rows = routes_ref.shape[0]
    share = own_ref.shape[1]
    slots = experts * capacity
    wide = max(128, experts)
    tp = lax.axis_index("tp")
    lane = iota((rows, wide), 1)
    first = routes_ref[:, 0:1]
    second = routes_ref[:, 1:2]
    is_first = lane == first
    is_second = lane == second
    members = jnp.where(is_first, 1.0, 0.0) + jnp.where(is_second, 1.0, 0.0)
    row, col = iota((rows, rows), 0), iota((rows, rows), 1)
    before = bmm((col < row).astype(F32), members, (1, 0))
    slot = iota((rows, slots), 1)

    def spread(chosen, mine):
        rank = jnp.sum(jnp.where(mine, before, 0.0), axis=1, keepdims=True).astype(jnp.int32)
        target = jnp.where(rank < capacity, chosen * capacity + rank, -1)
        return jnp.where(slot == target, 1.0, 0.0)

    one = spread(first, is_first)
    two = spread(second, is_second)
    own = grad_ref[:, pl.ds(pl.multiple_of(tp * share, 128), share)]
    own_ref[...] = own
    wide_own = own.astype(F32)
    left = (wide_own * weight_ref[:, 0:1]).astype(BF16)
    right = (wide_own * weight_ref[:, 1:2]).astype(BF16)
    out_ref[...] = (bmm(one, left, (0, 0)) + bmm(two, right, (0, 0))).astype(BF16)
    spread_ref[...] = (one + two).astype(BF16)


def ends_kernel(k_ref, v_ref, fwd_ref, bwd_ref, out_ref):
    length, lanes = k_ref.shape
    rising, falling = cumulative(fwd_ref, bwd_ref)
    fwd_total = rising[length - 1 : length]
    bwd_total = falling[0:1]
    k = k_ref[...].astype(F32)
    kf = k * jnp.exp(fwd_total - rising)
    kb = k * jnp.exp(bwd_total - falling)
    fend = jnp.zeros((DV, lanes), F32)
    bend = jnp.zeros((DV, lanes), F32)
    for h in range(lanes // KEY_CHANNELS):
        v = v_ref[:, h * DV : (h + 1) * DV]
        fend = fend + bmm(v, masked(h, kf), (0, 0))
        bend = bend + bmm(v, masked(h, kb), (0, 0))
    put_chunks(out_ref, fend, bend, fwd_total, bwd_total, True)


def block_factors(b, rising, falling):
    s = b * BLOCK
    fmid = rising[s + BLOCK // 2 - 1 : s + BLOCK // 2]
    bmid = falling[s + BLOCK // 2 : s + BLOCK // 2 + 1]
    block = slice(s, s + BLOCK)
    return (
        jnp.exp(rising[block] - fmid),
        jnp.exp(jnp.minimum(fmid - rising, 64.0)),
        jnp.exp(falling[block] - bmid),
        jnp.exp(jnp.minimum(bmid - falling, 64.0)),
    )


def causal(b, length):
    return iota((BLOCK, length), 1) <= iota((BLOCK, length), 0) + b * BLOCK


def forward_kernel(in_ref, q_ref, k_ref, v_ref, fwd_ref, bwd_ref, score_ref, o_ref, rows_ref, s_ref, r_ref):
    length, lanes = q_ref.shape
    heads = lanes // KEY_CHANNELS
    entry, back_entry = take_chunks(in_ref)
    s_ref[...] = entry
    r_ref[...] = back_entry
    rising, falling = cumulative(fwd_ref, bwd_ref)
    q = q_ref[...].astype(F32) * SCALE
    k = k_ref[...].astype(F32)
    for b in range(length // BLOCK):
        block = slice(b * BLOCK, (b + 1) * BLOCK)
        fq, fk, bq, bk = block_factors(b, rising, falling)
        qf = q[block] * fq
        qb = q[block] * bq
        kf = (k * fk).astype(BF16)
        kb = (k * bk).astype(BF16)
        keep = causal(b, length)
        for h in range(heads):
            fs = bmm(masked(h, qf), kf, (1, 1))
            bs = bmm(masked(h, qb), kb, (1, 1))
            score_ref[h, block, :] = jnp.where(keep, fs, bs).astype(BF16)
    qs = q * jnp.exp(rising)
    qr = q * jnp.exp(falling)
    for h in range(heads):
        cols = slice(h * DV, (h + 1) * DV)
        o = mm(score_ref[h], v_ref[:, cols], (1, 0))
        o = o + bmm(masked(h, qs), entry, (1, 1)) + bmm(masked(h, qr), back_entry, (1, 1))
        o_ref[:, cols] = o
        rms = lax.rsqrt(jnp.mean(o * o, axis=1, keepdims=True) + EPSILON)
        rows_ref[:, cols] = (o * rms).astype(BF16)


def cotangent_kernel(*refs, parts):
    streams = refs[:parts]
    proj_ref, o_ref, q_ref, fwd_ref, bwd_ref, do_ref, out_ref, column_ref = refs[parts:]
    length, lanes = q_ref.shape
    share = streams[0].shape[1]
    tp = lax.axis_index("tp")
    grad = jnp.zeros(o_ref.shape, F32)
    for m in range(parts):
        first = pl.multiple_of((tp ^ m) * share, 128)
        grad = grad + mm(streams[m][...], proj_ref[pl.ds(first, share), :], (1, 0))
        each = column_ref.shape[2]
        for i in range(share // each):
            place = (tp ^ m) * (share // each) + i
            column_ref[pl.ds(place, 1)] = streams[m][:, i * each : (i + 1) * each][None]
    rising, falling = cumulative(fwd_ref, bwd_ref)
    q = q_ref[...].astype(F32) * SCALE
    qs = q * jnp.exp(rising)
    qr = q * jnp.exp(falling)
    ds = jnp.zeros((DV, lanes), F32)
    dr = jnp.zeros((DV, lanes), F32)
    for h in range(lanes // KEY_CHANNELS):
        cols = slice(h * DV, (h + 1) * DV)
        o = o_ref[:, cols]
        rms = lax.rsqrt(jnp.mean(o * o, axis=1, keepdims=True) + EPSILON)
        mixed = o * rms
        dm = grad[:, cols]
        do = (rms * (dm - mixed * jnp.mean(dm * mixed, axis=1, keepdims=True))).astype(BF16)
        do_ref[:, cols] = do
        ds = ds + bmm(do, masked(h, qs), (0, 0))
        dr = dr + bmm(do, masked(h, qr), (0, 0))
    put_chunks(out_ref, ds, dr, rising[length - 1 : length], falling[0:1], False)


def weight_kernel(x_ref, gate_ref, up_ref, gate_out, up_out):
    gate_out[...] = mm(x_ref[...], gate_ref[...], (0, 0)).astype(BF16)
    up_out[...] = mm(x_ref[...], up_ref[...], (0, 0)).astype(BF16)


def weight_grads(x, gate_delta, up_delta, tile):
    slots, width = x.shape
    hidden = gate_delta.shape[1]
    out = jax.ShapeDtypeStruct((width, hidden), BF16)
    whole = pl.BlockSpec((slots, hidden), lambda i: (0, 0))
    return pl.pallas_call(
        weight_kernel,
        out_shape=(out, out),
        grid=(width // tile,),
        in_specs=[pl.BlockSpec((slots, tile), lambda i: (0, i)), whole, whole],
        out_specs=(pl.BlockSpec((tile, hidden), lambda i: (i, 0)),) * 2,
        cost_estimate=pl.CostEstimate(flops=3 * 10**9, bytes_accessed=5 << 20, transcendentals=0),
    )(x, gate_delta, up_delta)


def down_kernel(act_ref, *refs):
    pieces, out_ref = refs[:-1], refs[-1]
    tp = lax.axis_index("tp")
    share = pieces[0].shape[1]
    for m, piece in enumerate(pieces):
        first = pl.multiple_of((tp ^ m) * share, 128)
        out_ref[:, pl.ds(first, share)] = mm(act_ref[...], piece[...], (0, 0)).astype(BF16)


def final_kernel(
    cot_ref,
    column_ref,
    mixed_ref,
    do_ref,
    score_ref,
    q_ref,
    k_ref,
    v_ref,
    fwd_ref,
    bwd_ref,
    s_ref,
    r_ref,
    dq_ref,
    dk_ref,
    dv_ref,
    proj_ref,
    cot_in,
    column_in,
    dv_near,
    cot_send,
    cot_recv,
    column_send,
    column_recv,
):
    n = cot_ref.shape[0]
    greet(n)
    cot_copies = send_all(n, cot_ref, cot_in, cot_send, cot_recv)
    column_copies = send_all(n, column_ref, column_in, column_send, column_recv)
    keep_own(cot_ref, cot_in)
    keep_own(column_ref, column_in)
    length, lanes = q_ref.shape
    heads = lanes // KEY_CHANNELS
    rising, falling = cumulative(fwd_ref, bwd_ref)
    q = q_ref[...].astype(F32) * SCALE
    k = k_ref[...].astype(F32)
    dk = jnp.zeros((length, lanes), F32)
    reach = jnp.zeros((length, lanes), F32)
    reach_back = jnp.zeros((length, lanes), F32)
    for h in range(heads):
        cols = slice(h * DV, (h + 1) * DV)
        do = do_ref[:, cols]
        dv_near[:, cols] = mm(score_ref[h], do, (0, 0))
        reach = reach + bmm(do, masked(h, s_ref[...]), (1, 0))
        reach_back = reach_back + bmm(do, masked(h, r_ref[...]), (1, 0))
    far = reach * jnp.exp(rising) + reach_back * jnp.exp(falling)
    for b in range(length // BLOCK):
        block = slice(b * BLOCK, (b + 1) * BLOCK)
        fq, fk, bq, bk = block_factors(b, rising, falling)
        qf = q[block] * fq
        qb = q[block] * bq
        kf = k * fk
        kb = k * bk
        keep = causal(b, length)
        dqf = jnp.zeros((BLOCK, lanes), F32)
        dqb = jnp.zeros((BLOCK, lanes), F32)
        dkf = jnp.zeros((length, lanes), F32)
        dkb = jnp.zeros((length, lanes), F32)
        for h in range(heads):
            cols = slice(h * DV, (h + 1) * DV)
            dscore = mm(do_ref[block, cols], v_ref[:, cols], (1, 1))
            df = jnp.where(keep, dscore, 0.0).astype(BF16)
            db = jnp.where(keep, 0.0, dscore).astype(BF16)
            dqf = dqf + bmm(df, masked(h, kf), (1, 0))
            dqb = dqb + bmm(db, masked(h, kb), (1, 0))
            dkf = dkf + bmm(df, masked(h, qf), (0, 0))
            dkb = dkb + bmm(db, masked(h, qb), (0, 0))
        dq_ref[block, :] = ((dqf * fq + dqb * bq + far[block]) * SCALE).astype(BF16)
        dk = dk + dkf * fk + dkb * bk
    for copy in cot_copies:
        copy.wait()
    earlier, later = take_chunks(cot_in)
    ff = jnp.exp(rising[length - 1 : length] - rising)
    bf = jnp.exp(falling[0:1] - falling)
    kf = k * ff
    kb = k * bf
    ahead = jnp.zeros((length, lanes), F32)
    behind = jnp.zeros((length, lanes), F32)
    for h in range(lanes // KEY_CHANNELS):
        cols = slice(h * DV, (h + 1) * DV)
        v = v_ref[:, cols]
        ahead = ahead + bmm(v, masked(h, later), (1, 0))
        behind = behind + bmm(v, masked(h, earlier), (1, 0))
        dv = dv_near[:, cols] + bmm(masked(h, kf), later, (1, 1)) + bmm(masked(h, kb), earlier, (1, 1))
        dv_ref[:, cols] = dv.astype(BF16)
    dk_ref[...] = (dk + ahead * ff + behind * bf).astype(BF16)
    for copy in column_copies:
        copy.wait()
    total = jnp.zeros(proj_ref.shape, F32)
    for source in range(n):
        total = total + mm(column_in[source], mixed_ref[source], (0, 0))
    proj_ref[...] = total


def exchange(array):
    return lax.all_to_all(array, "sp", split_axis=0, concat_axis=0, tiled=True)


def on_device(
    layer_grad,
    routes,
    route_weight,
    slot_tokens,
    gate_proj,
    up_proj,
    down_proj,
    out_proj,
    queries,
    keys,
    values,
    fwd_decay,
    bwd_decay,
):
    sds = jax.ShapeDtypeStruct
    devices = lax.axis_size("sp")
    parts = lax.axis_size("tp")
    tp = lax.axis_index("tp")
    rows, width = layer_grad.shape
    slots = slot_tokens.shape[1]
    capacity = slots // devices
    share = width // parts
    lanes = keys.shape[1]
    heads = lanes // KEY_CHANNELS
    vwidth = values.shape[1]

    def swap(array, bit):
        return lax.ppermute(array, "tp", [(i, i ^ bit) for i in range(parts)])

    def gather_parts(own):
        pieces = {0: own}
        bit = parts // 2
        while bit:
            for m in list(pieces):
                pieces[m ^ bit] = swap(pieces[m], bit)
            bit //= 2
        return [pieces[m] for m in range(parts)]

    outgoing, spread, own_grad = call(
        functools.partial(dispatch_kernel, experts=devices, capacity=capacity),
        (sds((slots, share), BF16), sds((rows, slots), BF16), sds((rows, share), BF16)),
        (8 * rows * slots * share, 3 << 20),
        routes,
        route_weight,
        layer_grad,
    )
    chunk = sds((devices, DV + TAIL, lanes), BF16)
    ends = call(ends_kernel, chunk, (2 * 10**9, 3 << 20), keys, values, fwd_decay, bwd_decay)
    arrived, states = exchange_many(0, outgoing.reshape(devices, capacity, share), ends)
    inbound = gather_parts(arrived.reshape(slots, share))

    x = slot_tokens[0]
    w_gate, w_up, w_down = gate_proj[0], up_proj[0], down_proj[0]
    gate = jnp.dot(x, w_gate, preferred_element_type=F32)
    upper = jnp.dot(x, w_up, preferred_element_type=F32)
    sigma = jax.nn.sigmoid(gate)
    act = (gate * sigma * upper).astype(BF16)

    scores, o, mixed_rows, entry, back_entry = call(
        forward_kernel,
        (
            sds((heads, rows, rows), BF16),
            sds((rows, vwidth), F32),
            sds((rows, vwidth), BF16),
            sds((DV, lanes), F32),
            sds((DV, lanes), F32),
        ),
        (4 * 10**9, 3 << 20),
        states,
        queries,
        keys,
        values,
        fwd_decay,
        bwd_decay,
    )

    everyone = exchange(jnp.broadcast_to(mixed_rows[None], (devices, rows, vwidth)))
    last = inbound[1], inbound[parts - 1], mixed_rows, gate, upper
    inbound[1], inbound[parts - 1], mixed_rows, gate, upper = lax.optimization_barrier(last)
    act_grad = 0.0
    for m in range(parts):
        w = lax.dynamic_slice_in_dim(w_down, (tp ^ m) * share, share, 1)
        act_grad = act_grad + mm(inbound[m], w, (1, 1))
    up_delta = (act_grad * gate * sigma).astype(BF16)
    gate_delta = (act_grad * upper * sigma * (1.0 + gate * (1.0 - sigma))).astype(BF16)

    def slot_piece(m):
        wg = lax.dynamic_slice_in_dim(w_gate, (tp ^ m) * share, share, 0)
        wu = lax.dynamic_slice_in_dim(w_up, (tp ^ m) * share, share, 0)
        return (mm(gate_delta, wg, (1, 1)) + mm(up_delta, wu, (1, 1))).astype(BF16)

    pieces = {m: slot_piece(m) for m in reversed(range(parts))}
    bit = 1
    while bit < parts:
        kept = [m for m in pieces if not m & bit]
        got = {m: swap(pieces[m ^ bit], bit) for m in kept}
        bit *= 2
        if bit == parts:
            grad_gate, grad_up = weight_grads(x, gate_delta, up_delta, share)
            grad_down = call(
                down_kernel, sds(w_down.shape, BF16), (2 * 10**9, 4 << 20), act, *inbound
            )
            got[0], grad_gate, grad_up, grad_down = lax.optimization_barrier(
                (got[0], grad_gate, grad_up, grad_down)
            )
        pieces = {m: (pieces[m].astype(F32) + got[m].astype(F32)).astype(BF16) for m in kept}
    back = exchange_many(1, pieces[0].reshape(devices, capacity, share))[0].reshape(slots, share)

    stream = (own_grad.astype(F32) + mm(spread, back, (1, 0))).astype(BF16)
    streams = gather_parts(stream)
    do, cots, columns = call(
        functools.partial(cotangent_kernel, parts=parts),
        (sds((rows, vwidth), BF16), chunk, sds((devices, rows, width // devices), BF16)),
        (2 * 10**9, 4 << 20),
        *streams,
        out_proj,
        o,
        queries,
        fwd_decay,
        bwd_decay,
    )
    dq, dk, dv, proj_grad = call(
        final_kernel,
        (
            sds((rows, lanes), BF16),
            sds((rows, lanes), BF16),
            sds((rows, vwidth), BF16),
            sds((width // devices, vwidth), F32),
        ),
        (4 * 10**9, 8 << 20),
        cots,
        columns,
        everyone,
        do,
        scores,
        queries,
        keys,
        values,
        fwd_decay,
        bwd_decay,
        entry,
        back_entry,
        scratch_shapes=[
            pltpu.VMEM(cots.shape, BF16),
            pltpu.VMEM(columns.shape, BF16),
            pltpu.VMEM((rows, vwidth), F32),
        ]
        + sems(devices, 2),
        compiler_params=send_params(2),
    )
    return (grad_gate[None], grad_up[None], grad_down[None], proj_grad, dq, dk, dv)


def solution(mesh):
    placed = (
        P("sp", None),
        P("sp", None),
        P("sp", None),
        P("sp", None, None),
        P("sp", None, "tp"),
        P("sp", None, "tp"),
        P("sp", "tp", None),
        P(None, "tp"),
        P("sp", "tp"),
        P("sp", "tp"),
        P("sp", "tp"),
        P("sp", "tp"),
        P("sp", "tp"),
    )
    return jax.shard_map(
        on_device,
        mesh=mesh,
        in_specs=placed,
        out_specs=(
            P("sp", None, "tp"),
            P("sp", None, "tp"),
            P("sp", "tp", None),
            P("sp", "tp"),
            P("sp", "tp"),
            P("sp", "tp"),
            P("sp", "tp"),
        ),
        check_vma=False,
    )
```

```python
import functools

import jax
import jax.numpy as jnp
from jax import lax
from jax.experimental import pallas as pl
from jax.experimental.pallas import tpu as pltpu
from jax.sharding import PartitionSpec as P

KEY_CHANNELS = 64
DV = 128
BLOCK = 64
EPSILON = 1e-06
SCALE = KEY_CHANNELS ** (-0.5)
TAIL = 16
F32 = jnp.float32
BF16 = jnp.bfloat16
HIGHEST = lax.Precision.HIGHEST


def mm(a, b, contract, precision=None):
    return lax.dot_general(
        a, b, ((contract[:1], contract[1:]), ((), ())), preferred_element_type=F32, precision=precision
    )


def bmm(a, b, contract):
    return mm(a.astype(BF16), b.astype(BF16), contract)


def call(kernel, outs, cost, *args, **scratch):
    flops, nbytes = cost
    return pl.pallas_call(
        kernel,
        out_shape=outs,
        in_specs=[pl.BlockSpec(memory_space=pltpu.VMEM)] * len(args),
        out_specs=jax.tree.map(lambda _: pl.BlockSpec(memory_space=pltpu.VMEM), outs),
        cost_estimate=pl.CostEstimate(flops=flops, bytes_accessed=nbytes, transcendentals=0),
        **scratch,
    )(*args)


def iota(shape, dim):
    return lax.broadcasted_iota(jnp.int32, shape, dim)


def cumulative(fwd_ref, bwd_ref):
    length = fwd_ref.shape[0]
    row, col = iota((length, length), 0), iota((length, length), 1)
    rising = mm((col <= row).astype(F32), fwd_ref[...], (1, 0), HIGHEST)
    falling = mm((col >= row).astype(F32), bwd_ref[...], (1, 0), HIGHEST)
    return rising, falling


def head_mask(h, shape):
    return (iota(shape, 1) // KEY_CHANNELS) == h


def masked(h, array):
    return jnp.where(head_mask(h, array.shape), array, jnp.zeros_like(array))


def put_chunks(out_ref, fwd_state, bwd_state, fwd_total, bwd_total, forward_up):
    n = out_ref.shape[0]
    me = lax.axis_index("sp")
    lanes = out_ref.shape[2]

    def packed(state, total):
        hi = total.astype(BF16)
        rest = total - hi.astype(F32)
        mid = rest.astype(BF16)
        low = (rest - mid.astype(F32)).astype(BF16)
        row = iota((TAIL, lanes), 0)
        wide = lambda a: jnp.broadcast_to(a.astype(F32), (TAIL, lanes))
        tail = jnp.where(
            row == 0, wide(hi), jnp.where(row == 1, wide(mid), jnp.where(row == 2, wide(low), 0.0))
        )
        return state, tail

    fstate, ftail = packed(fwd_state, fwd_total)
    bstate, btail = packed(bwd_state, bwd_total)

    def one(d, carry):
        up = (d > me) if forward_up else (d < me)
        out_ref[pl.ds(d, 1), 0:DV, :] = jnp.where(up, fstate, bstate).astype(BF16)[None]
        out_ref[pl.ds(d, 1), DV : DV + TAIL, :] = jnp.where(up, ftail, btail).astype(BF16)[None]
        return carry

    lax.fori_loop(0, n, one, 0)


def take_chunks(in_ref):
    n, _, lanes = in_ref.shape
    me = lax.axis_index("sp")

    def piece(s):
        state = in_ref[pl.ds(s, 1), 0:DV, :][0].astype(F32)
        tail = in_ref[pl.ds(s, 1), DV : DV + TAIL, :][0].astype(F32)
        total = tail[0:1] + tail[1:2] + tail[2:3]
        return state, jnp.exp(total)

    def ahead(s, state):
        fresh, decay = piece(s)
        return jnp.where(s < me, state * decay + fresh, state)

    def behind(hop, state):
        s = n - 1 - hop
        fresh, decay = piece(s)
        return jnp.where(s > me, state * decay + fresh, state)

    zero = jnp.zeros((DV, lanes), F32)
    return lax.fori_loop(0, n, ahead, zero), lax.fori_loop(0, n, behind, zero)


def peers(n):
    me = lax.axis_index("sp")
    return me, [lax.rem(me + hop, n) for hop in range(1, n)]


def greet(n, more=0):
    _, others = peers(n)
    barrier = pltpu.get_barrier_semaphore()
    for other in others:
        pl.semaphore_signal(
            barrier, inc=1, device_id={"sp": other}, device_id_type=pl.DeviceIdType.MESH
        )
    pl.semaphore_wait(barrier, n - 1 + more)


def send_all(n, source, landing, send_sem, recv_sem):
    me, others = peers(n)
    copies = []
    for hop, other in enumerate(others):
        copy = pltpu.make_async_remote_copy(
            src_ref=source.at[other],
            dst_ref=landing.at[me],
            send_sem=send_sem.at[hop],
            recv_sem=recv_sem.at[hop],
            device_id={"sp": other},
            device_id_type=pl.DeviceIdType.MESH,
        )
        copy.start()
        copies.append(copy)
    return copies


def keep_own(source, landing):
    me = lax.axis_index("sp")
    landing[pl.ds(me, 1)] = source[pl.ds(me, 1)]


def exchange_kernel(*refs, arrays):
    sources, landings, sems = refs[:arrays], refs[arrays : 2 * arrays], refs[2 * arrays :]
    n = sources[0].shape[0]
    greet(n)
    copies = []
    for i in range(arrays):
        copies += send_all(n, sources[i], landings[i], sems[2 * i], sems[2 * i + 1])
    for source, landing in zip(sources, landings):
        keep_own(source, landing)
    for copy in copies:
        copy.wait()


def sems(n, arrays):
    return [pltpu.SemaphoreType.DMA((n - 1,)) for _ in range(2 * arrays)]


def send_params(number):
    return pltpu.CompilerParams(collective_id=number, has_side_effects=True)


def exchange_many(number, *arrays):
    n = arrays[0].shape[0]
    return call(
        functools.partial(exchange_kernel, arrays=len(arrays)),
        tuple(jax.ShapeDtypeStruct(a.shape, a.dtype) for a in arrays),
        (2 * 10**9, 8 << 20),
        *arrays,
        scratch_shapes=sems(n, len(arrays)),
        compiler_params=send_params(number),
    )


def dispatch_kernel(routes_ref, weight_ref, grad_ref, out_ref, spread_ref, own_ref, *, experts, capacity):
    rows = routes_ref.shape[0]
    share = own_ref.shape[1]
    slots = experts * capacity
    wide = max(128, experts)
    tp = lax.axis_index("tp")
    lane = iota((rows, wide), 1)
    first = routes_ref[:, 0:1]
    second = routes_ref[:, 1:2]
    is_first = lane == first
    is_second = lane == second
    members = jnp.where(is_first, 1.0, 0.0) + jnp.where(is_second, 1.0, 0.0)
    row, col = iota((rows, rows), 0), iota((rows, rows), 1)
    before = bmm((col < row).astype(F32), members, (1, 0))
    slot = iota((rows, slots), 1)

    def spread(chosen, mine):
        rank = jnp.sum(jnp.where(mine, before, 0.0), axis=1, keepdims=True).astype(jnp.int32)
        target = jnp.where(rank < capacity, chosen * capacity + rank, -1)
        return jnp.where(slot == target, 1.0, 0.0)

    one = spread(first, is_first)
    two = spread(second, is_second)
    own = grad_ref[:, pl.ds(pl.multiple_of(tp * share, 128), share)]
    own_ref[...] = own
    wide_own = own.astype(F32)
    left = (wide_own * weight_ref[:, 0:1]).astype(BF16)
    right = (wide_own * weight_ref[:, 1:2]).astype(BF16)
    out_ref[...] = (bmm(one, left, (0, 0)) + bmm(two, right, (0, 0))).astype(BF16)
    spread_ref[...] = (one + two).astype(BF16)


def ends_kernel(k_ref, v_ref, fwd_ref, bwd_ref, out_ref):
    length, lanes = k_ref.shape
    rising, falling = cumulative(fwd_ref, bwd_ref)
    fwd_total = rising[length - 1 : length]
    bwd_total = falling[0:1]
    k = k_ref[...].astype(F32)
    kf = k * jnp.exp(fwd_total - rising)
    kb = k * jnp.exp(bwd_total - falling)
    fend = jnp.zeros((DV, lanes), F32)
    bend = jnp.zeros((DV, lanes), F32)
    for h in range(lanes // KEY_CHANNELS):
        v = v_ref[:, h * DV : (h + 1) * DV]
        fend = fend + bmm(v, masked(h, kf), (0, 0))
        bend = bend + bmm(v, masked(h, kb), (0, 0))
    put_chunks(out_ref, fend, bend, fwd_total, bwd_total, True)


def block_factors(b, rising, falling):
    s = b * BLOCK
    fmid = rising[s + BLOCK // 2 - 1 : s + BLOCK // 2]
    bmid = falling[s + BLOCK // 2 : s + BLOCK // 2 + 1]
    block = slice(s, s + BLOCK)
    return (
        jnp.exp(rising[block] - fmid),
        jnp.exp(jnp.minimum(fmid - rising, 64.0)),
        jnp.exp(falling[block] - bmid),
        jnp.exp(jnp.minimum(bmid - falling, 64.0)),
    )


def causal(b, length):
    return iota((BLOCK, length), 1) <= iota((BLOCK, length), 0) + b * BLOCK


def forward_kernel(in_ref, q_ref, k_ref, v_ref, fwd_ref, bwd_ref, score_ref, o_ref, rows_ref, s_ref, r_ref):
    length, lanes = q_ref.shape
    heads = lanes // KEY_CHANNELS
    entry, back_entry = take_chunks(in_ref)
    s_ref[...] = entry
    r_ref[...] = back_entry
    rising, falling = cumulative(fwd_ref, bwd_ref)
    q = q_ref[...].astype(F32) * SCALE
    k = k_ref[...].astype(F32)
    for b in range(length // BLOCK):
        block = slice(b * BLOCK, (b + 1) * BLOCK)
        fq, fk, bq, bk = block_factors(b, rising, falling)
        qf = q[block] * fq
        qb = q[block] * bq
        kf = (k * fk).astype(BF16)
        kb = (k * bk).astype(BF16)
        keep = causal(b, length)
        for h in range(heads):
            fs = bmm(masked(h, qf), kf, (1, 1))
            bs = bmm(masked(h, qb), kb, (1, 1))
            score_ref[h, block, :] = jnp.where(keep, fs, bs).astype(BF16)
    qs = q * jnp.exp(rising)
    qr = q * jnp.exp(falling)
    for h in range(heads):
        cols = slice(h * DV, (h + 1) * DV)
        o = mm(score_ref[h], v_ref[:, cols], (1, 0))
        o = o + bmm(masked(h, qs), entry, (1, 1)) + bmm(masked(h, qr), back_entry, (1, 1))
        o_ref[:, cols] = o
        rms = lax.rsqrt(jnp.mean(o * o, axis=1, keepdims=True) + EPSILON)
        mixed = (o * rms).astype(BF16)
        for d in range(rows_ref.shape[0]):
            rows_ref[d, :, cols] = mixed


def cotangent_kernel(*refs, parts):
    streams = refs[:parts]
    proj_ref, o_ref, q_ref, fwd_ref, bwd_ref, do_ref, out_ref, column_ref = refs[parts:]
    length, lanes = q_ref.shape
    share = streams[0].shape[1]
    tp = lax.axis_index("tp")
    grad = jnp.zeros(o_ref.shape, F32)
    part = column_ref.shape[1]
    mine = pl.ds(pl.multiple_of(tp * part, 16), part)
    for m in range(parts):
        first = pl.multiple_of((tp ^ m) * share, 128)
        grad = grad + mm(streams[m][...], proj_ref[pl.ds(first, share), :], (1, 0))
        each = column_ref.shape[2]
        for i in range(share // each):
            place = (tp ^ m) * (share // each) + i
            column_ref[pl.ds(place, 1)] = streams[m][mine, i * each : (i + 1) * each][None]
    rising, falling = cumulative(fwd_ref, bwd_ref)
    q = q_ref[...].astype(F32) * SCALE
    qs = q * jnp.exp(rising)
    qr = q * jnp.exp(falling)
    ds = jnp.zeros((DV, lanes), F32)
    dr = jnp.zeros((DV, lanes), F32)
    for h in range(lanes // KEY_CHANNELS):
        cols = slice(h * DV, (h + 1) * DV)
        o = o_ref[:, cols]
        rms = lax.rsqrt(jnp.mean(o * o, axis=1, keepdims=True) + EPSILON)
        mixed = o * rms
        dm = grad[:, cols]
        do = (rms * (dm - mixed * jnp.mean(dm * mixed, axis=1, keepdims=True))).astype(BF16)
        do_ref[:, cols] = do
        ds = ds + bmm(do, masked(h, qs), (0, 0))
        dr = dr + bmm(do, masked(h, qr), (0, 0))
    put_chunks(out_ref, ds, dr, rising[length - 1 : length], falling[0:1], False)


def weight_kernel(x_ref, gate_ref, up_ref, gate_out, up_out):
    gate_out[...] = mm(x_ref[...], gate_ref[...], (0, 0)).astype(BF16)
    up_out[...] = mm(x_ref[...], up_ref[...], (0, 0)).astype(BF16)


def weight_grads(x, gate_delta, up_delta, tile):
    slots, width = x.shape
    hidden = gate_delta.shape[1]
    out = jax.ShapeDtypeStruct((width, hidden), BF16)
    whole = pl.BlockSpec((slots, hidden), lambda i: (0, 0))
    return pl.pallas_call(
        weight_kernel,
        out_shape=(out, out),
        grid=(width // tile,),
        in_specs=[pl.BlockSpec((slots, tile), lambda i: (0, i)), whole, whole],
        out_specs=(pl.BlockSpec((tile, hidden), lambda i: (i, 0)),) * 2,
        cost_estimate=pl.CostEstimate(flops=3 * 10**9, bytes_accessed=5 << 20, transcendentals=0),
    )(x, gate_delta, up_delta)


def down_kernel(act_ref, *refs):
    pieces, out_ref = refs[:-1], refs[-1]
    tp = lax.axis_index("tp")
    share = pieces[0].shape[1]
    for m, piece in enumerate(pieces):
        first = pl.multiple_of((tp ^ m) * share, 128)
        out_ref[:, pl.ds(first, share)] = mm(act_ref[...], piece[...], (0, 0)).astype(BF16)


def final_kernel(
    cot_ref,
    column_ref,
    mixed_ref,
    do_ref,
    score_ref,
    q_ref,
    k_ref,
    v_ref,
    fwd_ref,
    bwd_ref,
    s_ref,
    r_ref,
    dq_ref,
    dk_ref,
    dv_ref,
    proj_ref,
    cot_in,
    column_in,
    dv_near,
    cot_send,
    cot_recv,
    column_send,
    column_recv,
    gather_in,
    gather_send,
    gather_recv,
):
    n = cot_ref.shape[0]
    parts, _, part, each = gather_in.shape
    tp = lax.axis_index("tp")
    barrier = pltpu.get_barrier_semaphore()
    for m in range(1, parts):
        pl.semaphore_signal(
            barrier, inc=1, device_id={"tp": tp ^ m}, device_id_type=pl.DeviceIdType.MESH
        )
    greet(n, parts - 1)
    cot_copies = send_all(n, cot_ref, cot_in, cot_send, cot_recv)
    column_copies = send_all(n, column_ref, column_in, column_send, column_recv)
    keep_own(cot_ref, cot_in)
    keep_own(column_ref, column_in)
    length, lanes = q_ref.shape
    heads = lanes // KEY_CHANNELS
    rising, falling = cumulative(fwd_ref, bwd_ref)
    q = q_ref[...].astype(F32) * SCALE
    k = k_ref[...].astype(F32)
    dk = jnp.zeros((length, lanes), F32)
    reach = jnp.zeros((length, lanes), F32)
    reach_back = jnp.zeros((length, lanes), F32)
    for h in range(heads):
        cols = slice(h * DV, (h + 1) * DV)
        do = do_ref[:, cols]
        dv_near[:, cols] = mm(score_ref[h], do, (0, 0))
        reach = reach + bmm(do, masked(h, s_ref[...]), (1, 0))
        reach_back = reach_back + bmm(do, masked(h, r_ref[...]), (1, 0))
    far = reach * jnp.exp(rising) + reach_back * jnp.exp(falling)
    for b in range(length // BLOCK):
        block = slice(b * BLOCK, (b + 1) * BLOCK)
        fq, fk, bq, bk = block_factors(b, rising, falling)
        qf = q[block] * fq
        qb = q[block] * bq
        kf = k * fk
        kb = k * bk
        keep = causal(b, length)
        dqf = jnp.zeros((BLOCK, lanes), F32)
        dqb = jnp.zeros((BLOCK, lanes), F32)
        dkf = jnp.zeros((length, lanes), F32)
        dkb = jnp.zeros((length, lanes), F32)
        for h in range(heads):
            cols = slice(h * DV, (h + 1) * DV)
            dscore = mm(do_ref[block, cols], v_ref[:, cols], (1, 1))
            df = jnp.where(keep, dscore, 0.0).astype(BF16)
            db = jnp.where(keep, 0.0, dscore).astype(BF16)
            dqf = dqf + bmm(df, masked(h, kf), (1, 0))
            dqb = dqb + bmm(db, masked(h, kb), (1, 0))
            dkf = dkf + bmm(df, masked(h, qf), (0, 0))
            dkb = dkb + bmm(db, masked(h, qb), (0, 0))
        dq_ref[block, :] = ((dqf * fq + dqb * bq + far[block]) * SCALE).astype(BF16)
        dk = dk + dkf * fk + dkb * bk
    for copy in cot_copies:
        copy.wait()
    for copy in column_copies:
        copy.wait()
    relays = []
    for m in range(1, parts):
        copy = pltpu.make_async_remote_copy(
            src_ref=column_in,
            dst_ref=gather_in.at[tp],
            send_sem=gather_send.at[m - 1],
            recv_sem=gather_recv.at[m - 1],
            device_id={"tp": tp ^ m},
            device_id_type=pl.DeviceIdType.MESH,
        )
        copy.start()
        relays.append(copy)
    earlier, later = take_chunks(cot_in)
    ff = jnp.exp(rising[length - 1 : length] - rising)
    bf = jnp.exp(falling[0:1] - falling)
    kf = k * ff
    kb = k * bf
    ahead = jnp.zeros((length, lanes), F32)
    behind = jnp.zeros((length, lanes), F32)
    for h in range(lanes // KEY_CHANNELS):
        cols = slice(h * DV, (h + 1) * DV)
        v = v_ref[:, cols]
        ahead = ahead + bmm(v, masked(h, later), (1, 0))
        behind = behind + bmm(v, masked(h, earlier), (1, 0))
        dv = dv_near[:, cols] + bmm(masked(h, kf), later, (1, 1)) + bmm(masked(h, kb), earlier, (1, 1))
        dv_ref[:, cols] = dv.astype(BF16)
    dk_ref[...] = (dk + ahead * ff + behind * bf).astype(BF16)
    total = jnp.zeros(proj_ref.shape, F32)
    for m in range(parts):
        if m:
            relays[m - 1].wait()
            block = gather_in[tp ^ m]
        else:
            block = column_in[...]
        place = pl.ds(pl.multiple_of((tp ^ m) * part, 16), part)
        rows = mixed_ref[:, place, :].reshape(n * part, mixed_ref.shape[2])
        total = total + mm(block.reshape(n * part, each), rows, (0, 0))
    proj_ref[...] = total


def exchange(array):
    return lax.all_to_all(array, "sp", split_axis=0, concat_axis=0, tiled=True)


def on_device(
    layer_grad,
    routes,
    route_weight,
    slot_tokens,
    gate_proj,
    up_proj,
    down_proj,
    out_proj,
    queries,
    keys,
    values,
    fwd_decay,
    bwd_decay,
):
    sds = jax.ShapeDtypeStruct
    devices = lax.axis_size("sp")
    parts = lax.axis_size("tp")
    tp = lax.axis_index("tp")
    rows, width = layer_grad.shape
    slots = slot_tokens.shape[1]
    capacity = slots // devices
    share = width // parts
    lanes = keys.shape[1]
    heads = lanes // KEY_CHANNELS
    vwidth = values.shape[1]

    def swap(array, bit):
        return lax.ppermute(array, "tp", [(i, i ^ bit) for i in range(parts)])

    def gather_parts(own):
        pieces = {0: own}
        bit = parts // 2
        while bit:
            for m in list(pieces):
                pieces[m ^ bit] = swap(pieces[m], bit)
            bit //= 2
        return [pieces[m] for m in range(parts)]

    outgoing, spread, own_grad = call(
        functools.partial(dispatch_kernel, experts=devices, capacity=capacity),
        (sds((slots, share), BF16), sds((rows, slots), BF16), sds((rows, share), BF16)),
        (8 * rows * slots * share, 3 << 20),
        routes,
        route_weight,
        layer_grad,
    )
    chunk = sds((devices, DV + TAIL, lanes), BF16)
    ends = call(ends_kernel, chunk, (2 * 10**9, 3 << 20), keys, values, fwd_decay, bwd_decay)
    (arrived,) = exchange_many(0, outgoing.reshape(devices, capacity, share))
    states = exchange(ends)
    inbound = gather_parts(arrived.reshape(slots, share))

    x = slot_tokens[0]
    w_gate, w_up, w_down = gate_proj[0], up_proj[0], down_proj[0]
    gate = jnp.dot(x, w_gate, preferred_element_type=F32)
    upper = jnp.dot(x, w_up, preferred_element_type=F32)
    sigma = jax.nn.sigmoid(gate)
    act = (gate * sigma * upper).astype(BF16)

    scores, o, mixed_rows, entry, back_entry = call(
        forward_kernel,
        (
            sds((heads, rows, rows), BF16),
            sds((rows, vwidth), F32),
            sds((devices, rows, vwidth), BF16),
            sds((DV, lanes), F32),
            sds((DV, lanes), F32),
        ),
        (4 * 10**9, 3 << 20),
        states,
        queries,
        keys,
        values,
        fwd_decay,
        bwd_decay,
    )

    everyone = exchange(mixed_rows)
    last = inbound[1], inbound[parts - 1], mixed_rows, gate, upper
    inbound[1], inbound[parts - 1], mixed_rows, gate, upper = lax.optimization_barrier(last)
    act_grad = 0.0
    for m in range(parts):
        w = lax.dynamic_slice_in_dim(w_down, (tp ^ m) * share, share, 1)
        act_grad = act_grad + mm(inbound[m], w, (1, 1))
    up_delta = (act_grad * gate * sigma).astype(BF16)
    gate_delta = (act_grad * upper * sigma * (1.0 + gate * (1.0 - sigma))).astype(BF16)

    def slot_piece(m):
        wg = lax.dynamic_slice_in_dim(w_gate, (tp ^ m) * share, share, 0)
        wu = lax.dynamic_slice_in_dim(w_up, (tp ^ m) * share, share, 0)
        return (mm(gate_delta, wg, (1, 1)) + mm(up_delta, wu, (1, 1))).astype(BF16)

    pieces = {m: slot_piece(m) for m in reversed(range(parts))}
    bit = 1
    while bit < parts:
        kept = [m for m in pieces if not m & bit]
        got = {m: swap(pieces[m ^ bit], bit) for m in kept}
        bit *= 2
        if bit == parts:
            grad_gate, grad_up = weight_grads(x, gate_delta, up_delta, share)
            grad_down = call(
                down_kernel, sds(w_down.shape, BF16), (2 * 10**9, 4 << 20), act, *inbound
            )
            got[0], grad_gate, grad_up, grad_down = lax.optimization_barrier(
                (got[0], grad_gate, grad_up, grad_down)
            )
        pieces = {m: (pieces[m].astype(F32) + got[m].astype(F32)).astype(BF16) for m in kept}
    back = exchange_many(1, pieces[0].reshape(devices, capacity, share))[0].reshape(slots, share)

    stream = (own_grad.astype(F32) + mm(spread, back, (1, 0))).astype(BF16)
    streams = gather_parts(stream)
    do, cots, columns = call(
        functools.partial(cotangent_kernel, parts=parts),
        (sds((rows, vwidth), BF16), chunk, sds((devices, rows // parts, width // devices), BF16)),
        (2 * 10**9, 4 << 20),
        *streams,
        out_proj,
        o,
        queries,
        fwd_decay,
        bwd_decay,
    )
    dq, dk, dv, proj_grad = call(
        final_kernel,
        (
            sds((rows, lanes), BF16),
            sds((rows, lanes), BF16),
            sds((rows, vwidth), BF16),
            sds((width // devices, vwidth), F32),
        ),
        (4 * 10**9, 8 << 20),
        cots,
        columns,
        everyone,
        do,
        scores,
        queries,
        keys,
        values,
        fwd_decay,
        bwd_decay,
        entry,
        back_entry,
        scratch_shapes=[
            pltpu.VMEM(cots.shape, BF16),
            pltpu.VMEM(columns.shape, BF16),
            pltpu.VMEM((rows, vwidth), F32),
        ]
        + sems(devices, 2)
        + [
            pltpu.VMEM((parts,) + columns.shape, BF16),
            pltpu.SemaphoreType.DMA((parts - 1,)),
            pltpu.SemaphoreType.DMA((parts - 1,)),
        ],
        compiler_params=send_params(2),
    )
    return (grad_gate[None], grad_up[None], grad_down[None], proj_grad, dq, dk, dv)


def solution(mesh):
    placed = (
        P("sp", None),
        P("sp", None),
        P("sp", None),
        P("sp", None, None),
        P("sp", None, "tp"),
        P("sp", None, "tp"),
        P("sp", "tp", None),
        P(None, "tp"),
        P("sp", "tp"),
        P("sp", "tp"),
        P("sp", "tp"),
        P("sp", "tp"),
        P("sp", "tp"),
    )
    return jax.shard_map(
        on_device,
        mesh=mesh,
        in_specs=placed,
        out_specs=(
            P("sp", None, "tp"),
            P("sp", None, "tp"),
            P("sp", "tp", None),
            P("sp", "tp"),
            P("sp", "tp"),
            P("sp", "tp"),
            P("sp", "tp"),
        ),
        check_vma=False,
    )
```
